32 devices in a mesh: grp: 2 (over y), sp: 4 (over z), tp: 4 (over x, core).
Axes of the slice: x: 2, y: 2, z: 4, core: 2. Of those that a mesh axis runs over, the one named last changes fastest.
Arguments:
- queries: bfloat16 [1024, 2048], P(('grp', 'sp'), 'tp'), parts along dimension 0, may hold values from -8 to 8
- keys: bfloat16 [1024, 1024], P(('grp', 'sp'), 'tp'), parts along dimension 0, may hold values from -6 to 6
- values: bfloat16 [1024, 1024], P(('grp', 'sp'), 'tp'), parts along dimension 0, may hold values from -6 to 6
- head_bias: float32 [16], P('tp'), may hold values from -15 to -5
- documents: int32 [1024], P(('grp', 'sp')), parts along dimension 0, may hold values from 0 to 2, never falling along the last dimension, each value on 1 to 384 neighbouring positions
- w_out: bfloat16 [2048, 2048], P('tp'), may hold values from -0.125 to 0.125
- resid: bfloat16 [1024, 2048], P(('grp', 'sp', 'tp')), parts along dimension 0, may hold values from -6 to 6
- norm_gain: float32 [2048], replicated, may hold values from 0.1 to 1.9
- expert_ids: int32 [1024, 2], P(('grp', 'sp', 'tp')), parts along dimension 0, may hold values from 0 to 3, all different within a row; in each aligned block of 32 rows (0 to 31, 32 to 63, ...) at most 32 rows name the same one
- expert_gates: float32 [1024, 2], P(('grp', 'sp', 'tp')), parts along dimension 0, may hold values from 0.1 to 0.9
- w_gate: bfloat16 [4, 2048, 3072], P('sp', None, 'tp'), may hold values from -0.125 to 0.125
- w_up: bfloat16 [4, 2048, 3072], P('sp', None, 'tp'), may hold values from -0.125 to 0.125
- w_down: bfloat16 [4, 3072, 2048], P('sp', 'tp'), may hold values from -0.109375 to 0.109375
Outputs:
- layer_out: bfloat16 [1024, 2048], P(('grp', 'sp', 'tp')), parts along dimension 0
The draws below stay inside these ranges and needn't reach their ends.
There are 2 independent parts, one for each index of `grp`. The reference program is written for one: setup_inputs(seed, part) draws one part's arguments, and reference() takes and returns one part's arrays. A program takes and returns all parts, laid end to end along the dimension named above; an argument that names none is the same for every part. Nothing has to cross between parts.
Inputs may be any that keep to these rules, and one draw needn't show every extreme that they name: Document numbers never fall along the sequence; each of the 3 documents holds at least one position and the longest exactly 384 positions. `expert_ids`: each position names 2 different experts. Among the 32 positions of one device (aligned blocks of 32 rows) no expert is named more than 32 times, and in some block some expert exactly 32 times.
All inputs are finite; a program needn't handle non-finite values.
Results may differ from the reference program's by a relative error of at most 0.012.
Values may be sent and summed in bfloat16 or wider, within the bound.
A program may use at most 64 MiB of HBM per device.

```python
import math
import jax
import jax.numpy as jnp
import numpy as np
from jax import lax

D = 2048
HEADS = 16
KV_HEADS = 8
DH = 128
FF = 3072
TOPK = 2
DOCS = 3
SEQ = 512
ROWS = 32
EXPERTS = 4
CAP = 32
N_SP = 4
N_TP = 4


def draw_head_bias(key, part):
    return jax.random.uniform(key, (HEADS,), jnp.float32, -14.0, -5.0)


def shard_levels(own_key, dims, split, least, largest):
    gain, own = 1.0, jax.random.fold_in(own_key, 6)
    for axis_at, parts in split:
        steps = jnp.exp(jax.random.uniform(jax.random.fold_in(own, axis_at), (parts,), jnp.float32, least / len(split), largest / len(split)))
        gain = gain * jnp.repeat(steps, dims[axis_at] // parts).reshape([-1 if axis == axis_at else 1 for axis in range(len(dims))])
    return gain


def split_up(amount, total, reach, lean):
    loads = [(1 << 20) // math.isqrt(rank ** lean) + 1 for rank in range(2, amount + 1)]
    spare, holding = total - reach - (amount - 1), [1] * (amount - 1)
    while spare > 0:
        free = [i for i in range(amount - 1) if holding[i] < reach]
        whole, remaining = sum([loads[i] for i in free]), spare
        for i in free:
            extra = min(reach - holding[i], max(1, remaining * loads[i] // whole), spare)
            holding[i] = holding[i] + extra
            spare = spare - extra
    return np.array([reach] + holding)


def ragged_sizes(rng, count, total, reach, slope):
    if count == 2:
        one = jax.random.randint(rng, (), max(1, total - reach), min(reach, total - 1) + 1)
        return jnp.stack([one, total - one])
    sizes = jnp.asarray(split_up(count, total, reach, slope), jnp.int32)
    couples = (count - 1) // 2
    giver, taker = sizes[1:1 + 2 * couples:2], sizes[2:2 + 2 * couples:2]
    slack = jnp.minimum(giver - 1, reach - taker)
    shifted = jax.random.randint(jax.random.fold_in(rng, 1), (couples,), 0, 1 << 20) % (slack + 1)
    sizes = sizes.at[1:1 + 2 * couples:2].set(giver - shifted).at[2:2 + 2 * couples:2].set(taker + shifted)
    return sizes[jax.random.permutation(jax.random.fold_in(rng, 2), count)]


def assign_block(own_key, own, number, rows, number_of, top, most, slope):
    order = jax.random.permutation(own_key, number_of)
    packed, common = shares(number_of, rows * top, most, slope, True), shares(number_of, rows * top, most, slope, False)
    places = jnp.arange(number_of)

    def named(tallies, offset_by):
        used = int((tallies > 0).sum())
        fixed = max(1, used // 4)
        shifted = fixed + (places - fixed + offset_by * (used - fixed)) % max(1, number_of - fixed)
        return jnp.zeros((number_of,), jnp.int32).at[order[jnp.where(places < fixed, places, shifted)]].set(jnp.asarray(tallies, jnp.int32))

    tallies = jnp.where(number % 4 == 0, named(packed, number // 4), named(common, number - number // 4 - 1))
    mixed = jax.random.permutation(jax.random.fold_in(own, 3), number_of)
    donor, taker = mixed[0:number_of // 2 * 2:2], mixed[1:number_of // 2 * 2:2]
    room = jnp.minimum(tallies[donor] - 1, most - tallies[taker]) // 2
    room = jnp.where((donor == order[0]) | (taker == order[0]) | (tallies[taker] == 0), 0, jnp.maximum(room, 0))
    shifted = jax.random.randint(jax.random.fold_in(own, 4), (number_of // 2,), 0, 1 << 20) % (room + 1)
    tallies = tallies.at[donor].add(-shifted).at[taker].add(shifted)
    labels = jnp.searchsorted(jnp.cumsum(tallies), jnp.arange(rows * top), side="right").astype(jnp.int32)
    table = labels.reshape(top, rows).T
    table = table[jax.random.permutation(jax.random.fold_in(own, 1), rows)]
    offset_by = jax.random.randint(jax.random.fold_in(own, 2), (rows, 1), 0, top)
    return jnp.take_along_axis(table, (jnp.arange(top)[None, :] + offset_by) % top, axis=1)


def shares(amount, total, reach, skew, full):
    loads = [(1 << 20) // math.isqrt(grade ** skew) + 1 for grade in range(1, amount + 1)]
    largest = reach if full else min(reach, max(-(-total // amount), total * loads[0] // sum(loads)))
    least = 1 if total - largest >= amount - 1 else 0
    given, rest = [largest] + [least] * (amount - 1), total - largest - least * (amount - 1)
    while rest > 0:
        candidates = [i for i in range(1, amount) if given[i] < largest] or [i for i in range(1, amount) if given[i] < reach]
        whole, budget = sum([loads[i] for i in candidates]), rest
        for i in candidates:
            extra = min(reach - given[i], max(1, budget * loads[i] // whole), rest)
            given[i] = given[i] + extra
            rest = rest - extra
    return np.array(given)


def centred(own_key, shape, width, most, split=(), kind=jnp.bfloat16):
    result = jax.random.normal(own_key, shape, jnp.float32) * width
    if len(split) > 0:
        result = shard_levels(own_key, shape, split, -0.22, 0.18) * result
    return jnp.clip(result, min=-most, max=most).astype(kind)


def setup_inputs(seed: int = 0, part: int = 0) -> dict:
    key_list = jax.random.split(jax.random.key(seed), 14)
    own_keys = jax.random.split(jax.random.fold_in(key_list[13], part), 14)
    queries = centred(own_keys[0], (SEQ, HEADS * DH), 2.0, 8.0, ((0, 4), (1, 4)))
    keys = centred(own_keys[1], (SEQ, KV_HEADS * DH), 1.0, 6.0, ((0, 4), (1, 4)))
    values = centred(own_keys[2], (SEQ, KV_HEADS * DH), 1.0, 6.0, ((0, 4), (1, 4)))
    head_bias = draw_head_bias(jax.random.fold_in(key_list[13], 71), part)
    documents = jnp.searchsorted(jnp.cumsum(ragged_sizes(own_keys[4], DOCS, SEQ, 3 * SEQ // 4, 0)), jnp.arange(SEQ), side="right").astype(jnp.int32)
    w_out = centred(key_list[5], (HEADS * DH, D), (HEADS * DH) ** -0.5, 0.125, ((0, 4),))
    resid = centred(own_keys[6], (SEQ, D), 1.0, 6.0, ((0, 16),))
    norm_gain = jnp.clip(1.0 + 0.18 * jax.random.normal(key_list[7], (D,), jnp.float32), 0.1, 1.9)
    expert_ids_keys = jax.random.split(jax.random.fold_in(own_keys[8], 1), SEQ // ROWS)
    expert_ids_turns = jax.random.permutation(jax.random.fold_in(own_keys[8], 3), SEQ // ROWS)
    expert_ids = jax.vmap(lambda own, number: assign_block(jax.random.fold_in(own_keys[8], 2), own, number, ROWS, EXPERTS, TOPK, CAP, 1))(expert_ids_keys, expert_ids_turns).reshape((SEQ, TOPK))
    expert_gates = jnp.clip(0.1 + 0.79999997 * jax.random.uniform(own_keys[9], (SEQ, TOPK), jnp.float32) ** shard_levels(own_keys[9], (SEQ, TOPK), ((0, 16),), -0.2, 0.2), 0.1, 0.9)
    w_gate = centred(key_list[10], (EXPERTS, D, FF), D ** -0.5, 0.125, ((0, 4), (2, 4)))
    w_up = centred(key_list[11], (EXPERTS, D, FF), D ** -0.5, 0.125, ((0, 4), (2, 4)))
    w_down = centred(key_list[12], (EXPERTS, FF, D), FF ** -0.5, 0.109375, ((0, 4), (1, 4)))
    return {"queries": queries, "keys": keys, "values": values, "head_bias": head_bias, "documents": documents, "w_out": w_out, "resid": resid, "norm_gain": norm_gain, "expert_ids": expert_ids, "expert_gates": expert_gates, "w_gate": w_gate, "w_up": w_up, "w_down": w_down}


def rounded(array):
    return lax.optimization_barrier(array.astype(jnp.bfloat16)).astype(jnp.float32)

def reference(queries, keys, values, head_bias, documents, w_out, resid, norm_gain, expert_ids, expert_gates, w_gate, w_up, w_down):
    highest = lax.Precision.HIGHEST
    group_size = HEADS // KV_HEADS
    scale_factor = DH ** (-0.5)
    query_all = queries.astype(jnp.float32).reshape(SEQ, KV_HEADS, group_size, DH)
    key_all = keys.astype(jnp.float32).reshape(SEQ, KV_HEADS, DH)
    value_all = values.astype(jnp.float32).reshape(SEQ, KV_HEADS, DH)
    bias_grid = head_bias.astype(jnp.float32).reshape(KV_HEADS, group_size)
    positions = jnp.arange(SEQ, dtype=jnp.int32)
    block_rows = math.gcd(SEQ, 256)

    def attend_block(block_index):
        first = block_index * block_rows
        query_block = lax.dynamic_slice_in_dim(query_all, first, block_rows, 0)
        query_pos = first + jnp.arange(block_rows, dtype=jnp.int32)
        query_doc = lax.dynamic_slice_in_dim(documents, first, block_rows, 0)
        live = (positions[None, :] < query_pos[:, None]) & (documents[None, :] == query_doc[:, None])
        logits = jnp.einsum('qgrd,sgd->grqs', query_block, key_all, precision=highest) * scale_factor + bias_grid[:, :, None, None]
        keep = jnp.where(live, jax.nn.log_sigmoid(-logits), 0.0)
        after = lax.cumsum(keep, axis=3, reverse=True) - keep
        weight = rounded(jnp.where(live, jnp.exp(jax.nn.log_sigmoid(logits) + after), 0.0))
        mixed_block = jnp.einsum('grqs,sgd->qgrd', weight, value_all, precision=highest)
        return mixed_block.reshape(block_rows, HEADS * DH).astype(jnp.bfloat16)
    mixed = lax.map(attend_block, jnp.arange(SEQ // block_rows, dtype=jnp.int32)).reshape(SEQ, HEADS * DH)
    share = HEADS * DH // N_TP
    partials = jnp.einsum('sjc,jcd->sjd', mixed.astype(jnp.float32).reshape(SEQ, N_TP, share), w_out.astype(jnp.float32).reshape(N_TP, share, D), precision=highest)
    middle = (resid.astype(jnp.float32) + lax.optimization_barrier(jnp.sum(rounded(partials), axis=1))).astype(jnp.bfloat16)
    middle_value = middle.astype(jnp.float32)
    normed = (middle_value * lax.rsqrt(lax.optimization_barrier(jnp.mean(middle_value * middle_value, axis=1, keepdims=True)) + 1e-06) * norm_gain.astype(jnp.float32)).astype(jnp.bfloat16)
    assignments = SEQ * TOPK
    most_rows = N_SP * N_TP * CAP
    flat_ids = expert_ids.reshape(-1)
    hidden_share = FF // N_TP

    def run_expert(expert):
        picks = jnp.nonzero(flat_ids == expert, size=most_rows, fill_value=assignments)[0].astype(jnp.int32)
        source = normed[jnp.minimum(picks, assignments - 1) // TOPK].astype(jnp.float32)
        gate_value = jnp.dot(source, w_gate[expert].astype(jnp.float32), precision=highest)
        up_value = jnp.dot(source, w_up[expert].astype(jnp.float32), precision=highest)
        hidden = rounded(jax.nn.silu(gate_value) * up_value).reshape(most_rows, N_TP, hidden_share)
        partial_out = jnp.einsum('bjf,jfd->bjd', hidden, w_down[expert].astype(jnp.float32).reshape(N_TP, hidden_share, D), precision=highest)
        return (lax.optimization_barrier(jnp.sum(rounded(partial_out), axis=1)).astype(jnp.bfloat16), picks)
    outputs, picks_all = lax.map(run_expert, jnp.arange(EXPERTS, dtype=jnp.int32))
    routed = jnp.zeros((assignments, D), jnp.bfloat16).at[picks_all.reshape(-1)].set(outputs.reshape(-1, D), mode='drop')
    combined = lax.optimization_barrier(jnp.sum(expert_gates.astype(jnp.float32)[:, :, None] * routed.reshape(SEQ, TOPK, D).astype(jnp.float32), axis=1))
    return (middle_value + combined).astype(jnp.bfloat16)
```

```python
import functools

import jax
import jax.numpy as jnp
from jax import lax
from jax.experimental import pallas as pl
from jax.experimental.pallas import tpu as pltpu
from jax.sharding import PartitionSpec as P

D = 2048
HEADS = 16
KV_HEADS = 8
DH = 128
TOPK = 2


def passed_along(value, axis, steps):
    count = lax.axis_size(axis)
    initial, last = (max(0, -steps), min(count, count - steps))
    return lax.ppermute(value, axis, [(source, source + steps) for source in range(initial, last)])


def attend_terms(query_grid, bias_grid, key_block, value_block, live, carried):
    kv_local = bias_grid.shape[0]
    key_count = key_block.shape[0]
    logits = (
        jnp.einsum(
            "qgrd,sgd->grqs",
            query_grid,
            key_block.reshape(key_count, kv_local, DH),
            preferred_element_type=jnp.float32,
        )
        * DH ** (-0.5)
        + bias_grid[:, :, None, None]
    )
    keep = jnp.where(live, jax.nn.log_sigmoid(-logits), 0.0)
    after = lax.cumsum(keep, axis=3, reverse=True) - keep + carried[:, :, :, None]
    weight = jnp.where(live, jnp.exp(jax.nn.log_sigmoid(logits) + after), 0.0).astype(jnp.bfloat16)
    partial_mix = jnp.einsum(
        "grqs,sgd->qgrd",
        weight,
        value_block.reshape(key_count, kv_local, DH),
        preferred_element_type=jnp.float32,
    )
    return (partial_mix, jnp.sum(keep, axis=3))


def local(
    queries,
    keys,
    values,
    head_bias,
    documents,
    w_out,
    resid,
    norm_gain,
    expert_ids,
    expert_gates,
    w_gate,
    w_up,
    w_down,
):
    tok_count = queries.shape[0]
    kv_local = keys.shape[1] // DH
    group_size = HEADS // KV_HEADS
    sp_count = lax.axis_size("sp")
    tp_count = lax.axis_size("tp")
    sp_index = lax.axis_index("sp")
    query_grid = queries.reshape(tok_count, kv_local, group_size, DH)
    bias_grid = head_bias.reshape(kv_local, group_size)
    doc_here = documents.astype(jnp.bfloat16)
    doc_column = doc_here.reshape(tok_count, 1)
    local_pos = jnp.arange(tok_count, dtype=jnp.int32)
    live_local = (local_pos[None, :] < local_pos[:, None]) & (
        documents[None, :] == documents[:, None]
    )
    zero_carry = jnp.zeros((kv_local, group_size, tok_count), jnp.float32)
    mix_total, carried = attend_terms(query_grid, bias_grid, keys, values, live_local, zero_carry)

    def visit(turn_index, state):
        mix_sum, carry_sum, key_block, value_block, doc_block = state
        key_block, value_block, doc_block = passed_along(
            (key_block, value_block, doc_block), "sp", 1
        )
        live = (doc_block[:, 0][None, :] == doc_here[:, None]) & (sp_index - turn_index >= 0)
        partial_mix, block_keep = attend_terms(
            query_grid, bias_grid, key_block, value_block, live, carry_sum
        )
        return (mix_sum + partial_mix, carry_sum + block_keep, key_block, value_block, doc_block)

    mix_total, carried, key_last, value_last, doc_last = lax.fori_loop(
        1, sp_count, visit, (mix_total, carried, keys, values, doc_column)
    )
    mixed = mix_total.reshape(tok_count, kv_local * group_size * DH).astype(jnp.bfloat16)
    projected = lax.psum_scatter(
        jnp.dot(mixed, w_out, preferred_element_type=jnp.float32).astype(jnp.bfloat16),
        "tp",
        scatter_dimension=0,
        tiled=True,
    ).astype(jnp.float32)
    middle = (resid.astype(jnp.float32) + projected).astype(jnp.bfloat16)
    middle_value = middle.astype(jnp.float32)
    normed = (
        middle_value
        * lax.rsqrt(jnp.mean(middle_value * middle_value, axis=1, keepdims=True) + 1e-06)
        * norm_gain
    ).astype(jnp.bfloat16)
    row_count = normed.shape[0]
    expert_count = w_gate.shape[0] * sp_count
    slot_limit = min(row_count, max(2, 2 * TOPK * row_count // expert_count))
    flat_ids = expert_ids.reshape(-1)
    onehot_ids = (flat_ids[:, None] == jnp.arange(expert_count, dtype=jnp.int32)[None, :]).astype(
        jnp.int32
    )
    earlier = jnp.cumsum(onehot_ids, axis=0) - onehot_ids
    slot_ids = jnp.sum(earlier * onehot_ids, axis=1)
    target = flat_ids * slot_limit + slot_ids
    placing = (
        jnp.arange(expert_count * slot_limit, dtype=jnp.int32)[:, None] == target[None, :]
    ).astype(jnp.bfloat16)
    by_token = jnp.sum(placing.reshape(expert_count * slot_limit, row_count, TOPK), axis=2)
    outgoing = jnp.dot(by_token, normed, preferred_element_type=jnp.float32).astype(jnp.bfloat16)
    outgoing = outgoing.reshape(expert_count, slot_limit, D)
    arrived = lax.all_to_all(outgoing, "sp", split_axis=0, concat_axis=0, tiled=True)
    gathered = lax.all_gather(arrived, "tp", axis=0, tiled=True)
    expert_rows = gathered.reshape(-1, D)
    gate_value = jnp.dot(expert_rows, w_gate[0], preferred_element_type=jnp.float32)
    up_value = jnp.dot(expert_rows, w_up[0], preferred_element_type=jnp.float32)
    hidden = (jax.nn.silu(gate_value) * up_value).astype(jnp.bfloat16)
    partial_out = jnp.dot(hidden, w_down[0], preferred_element_type=jnp.float32)
    summed = lax.psum_scatter(
        partial_out.reshape(tp_count, sp_count * slot_limit, D).astype(jnp.bfloat16),
        "tp",
        scatter_dimension=0,
        tiled=True,
    ).astype(jnp.float32)
    expert_result = summed.reshape(sp_count, slot_limit, D).astype(jnp.bfloat16)
    returned = lax.all_to_all(expert_result, "sp", split_axis=0, concat_axis=0, tiled=True)
    routed = jnp.dot(placing.T, returned.reshape(-1, D), preferred_element_type=jnp.float32)
    combined = jnp.sum(expert_gates[:, :, None] * routed.reshape(row_count, TOPK, D), axis=1)
    return (middle_value + combined).astype(jnp.bfloat16)


MESH = pl.DeviceIdType.MESH


def paired(index, turn, count):
    result, bit = 0, 1
    while bit < count:
        a, b = lax.rem(index // bit, 2), lax.rem(turn // bit, 2)
        result = result + bit * (a + b - 2 * a * b)
        bit *= 2
    return result


def fused_kernel(
    sp_count,
    tp_count,
    q_ref,
    k_ref,
    v_ref,
    bias_ref,
    doc_ref,
    resid_ref,
    gain_ref,
    ids_ref,
    gates_ref,
    w_out_hbm,
    w_gate_hbm,
    w_up_hbm,
    w_down_hbm,
    out_ref,
    w_out,
    w_gate,
    w_up,
    w_down,
    k_all,
    v_all,
    doc_all,
    mix_acc,
    carry,
    mixed,
    middle,
    x_all,
    hidden,
    part,
    sib_in,
    x_out,
    x_in,
    z_out,
    returned,
    w_sem,
    kv_send,
    kv_recv,
    z_send,
    z_recv,
    gx_send,
    gx_recv,
    gs_send,
    gs_recv,
    ps_send,
    ps_recv,
    px_send,
    px_recv,
    rz_send,
    rz_recv,
):
    s = lax.axis_index("sp")
    t = lax.axis_index("tp")
    width = tp_count // 2
    x, c = t // 2, lax.rem(t, 2)
    sibling = 2 * x + 1 - c
    tok = q_ref.shape[0]
    kv_local = k_ref.shape[1] // DH
    rep = q_ref.shape[1] // k_ref.shape[1]
    rows, model = resid_ref.shape
    ff = w_up.shape[1]
    f32, bf16 = jnp.float32, jnp.bfloat16

    loads = [
        pltpu.make_async_copy(src, dst, w_sem.at[j])
        for j, (src, dst) in enumerate(
            (
                (w_out_hbm, w_out),
                (w_gate_hbm.at[0], w_gate),
                (w_up_hbm.at[0], w_up),
                (w_down_hbm.at[0], w_down),
            )
        )
    ]
    for load in loads:
        load.start()

    barrier = pltpu.get_barrier_semaphore()
    for j in range(1, sp_count):
        pl.semaphore_signal(
            barrier, inc=1, device_id={"sp": lax.rem(s + j, sp_count)}, device_id_type=MESH
        )
    for j in range(1, tp_count):
        pl.semaphore_signal(
            barrier, inc=1, device_id={"tp": lax.rem(t + j, tp_count)}, device_id_type=MESH
        )
    pl.semaphore_wait(barrier, sp_count + tp_count - 2)

    def remote(src, dst, send, recv, device):
        return pltpu.make_async_remote_copy(
            src_ref=src,
            dst_ref=dst,
            send_sem=send,
            recv_sem=recv,
            device_id=device,
            device_id_type=MESH,
        )

    def passed(hop):
        right = {"sp": lax.rem(s + 1, sp_count)}
        own = (k_ref, v_ref, doc_ref)
        slots = (k_all, v_all, doc_all)
        return [
            remote(
                own[j] if hop == 0 else slots[j].at[hop - 1],
                slots[j].at[hop],
                kv_send.at[hop, j],
                kv_recv.at[hop, j],
                right,
            )
            for j in range(3)
        ]

    has_right = s < sp_count - 1

    @pl.when(has_right)
    def _():
        for copy in passed(0):
            copy.start()

    at_row = lax.broadcasted_iota(jnp.int32, (tok, tok), 0)
    at_col = lax.broadcasted_iota(jnp.int32, (tok, tok), 1)
    summing = jnp.concatenate(
        [(at_row > at_col).astype(f32), jnp.ones((tok, tok), f32)], axis=1
    ).astype(bf16)
    doc_query = jnp.broadcast_to(doc_ref[...].astype(f32), (tok, tok)).T

    def attend(hop):
        docs = doc_ref[...] if hop == 0 else doc_all[hop - 1]
        live = doc_query == jnp.broadcast_to(docs.astype(f32), (tok, tok))
        if hop == 0:
            live = live & (at_col < at_row)
        live_f = jnp.concatenate([live.astype(f32)] * rep, axis=0)
        live_all = live_f > 0.5
        for g in range(kv_local):
            heads = [g * rep + r for r in range(rep)]
            query = jnp.concatenate([q_ref[:, h * DH : (h + 1) * DH] for h in heads], axis=0)
            bias = jnp.concatenate([jnp.full((tok, tok), bias_ref[h], f32) for h in heads], axis=0)
            lanes = slice(g * DH, (g + 1) * DH)
            key = k_ref[:, lanes] if hop == 0 else k_all[hop - 1, :, lanes]
            value = v_ref[:, lanes] if hop == 0 else v_all[hop - 1, :, lanes]
            logits = (
                lax.dot_general(
                    query, key, (((1,), (1,)), ((), ())), preferred_element_type=f32
                )
                * DH ** (-0.5)
                + bias
            )
            keep_any = -(jnp.maximum(logits, 0.0) + jnp.log1p(jnp.exp(-jnp.abs(logits))))
            keep = jnp.where(live_all, keep_any, 0.0)
            high = keep.astype(bf16)
            rest = keep - high.astype(f32)
            mid = rest.astype(bf16)
            low = (rest - mid.astype(f32)).astype(bf16)
            sums = (
                jnp.dot(high, summing, preferred_element_type=f32)
                + jnp.dot(mid, summing, preferred_element_type=f32)
                + jnp.dot(low, summing, preferred_element_type=f32)
            )
            after, total = sums[:, :tok], sums[:, tok:]
            if hop > 0:
                after = after + carry[g]
                total = total + carry[g]
            carry[g] = total
            weight = jnp.where(live_all, jnp.exp(logits + keep_any + after), 0.0).astype(bf16)
            mix = jnp.dot(weight, value, preferred_element_type=f32)
            mix_acc[g] = mix if hop == 0 else mix_acc[g] + mix

    attend(0)
    for hop in range(1, sp_count):

        @pl.when(s >= hop)
        def _():
            for copy in passed(hop - 1):
                copy.wait_recv()
            if hop < sp_count - 1:

                @pl.when(has_right)
                def _():
                    for copy in passed(hop):
                        copy.start()

            attend(hop)

    for g in range(kv_local):
        for r in range(rep):
            h = g * rep + r
            mixed[:, h * DH : (h + 1) * DH] = mix_acc[g, r * tok : (r + 1) * tok, :].astype(bf16)

    def pair_copies(i):
        return [
            remote(
                part.at[i, 2 * j + 1 - c],
                sib_in.at[i, j],
                ps_send.at[i, j],
                ps_recv.at[i, j],
                {"tp": sibling},
            )
            for j in range(width)
        ]

    def across_copies(i):
        return [
            remote(
                x_out.at[i, j - 1],
                x_in.at[i, j - 1],
                px_send.at[i, j - 1],
                px_recv.at[i, j - 1],
                {"tp": 2 * lax.rem(x + j, width) + c},
            )
            for j in range(1, width)
        ]

    def pair_sum(i, at):
        return part[i, 2 * at + c].astype(f32) + sib_in[i, at].astype(f32)

    def sum_pairs(i):
        for copy in pair_copies(i):
            copy.wait_recv()
        for j, copy in enumerate(across_copies(i)):
            x_out[i, j] = pair_sum(i, lax.rem(x + j + 1, width)).astype(bf16)
            copy.start()

    def sum_across(i):
        result = pair_sum(i, x)
        for j, copy in enumerate(across_copies(i)):
            copy.wait_recv()
            result = result + x_in[i, j].astype(f32)
        return result

    loads[0].wait()
    step = 512 if model % 512 == 0 else model

    def project(n, _):
        columns = pl.ds(pl.multiple_of(n * step, step), step)
        value = jnp.dot(mixed[...], w_out[:, columns], preferred_element_type=f32)
        part[sp_count, :, :, columns] = value.astype(bf16).reshape(tp_count, rows, step)
        return 0

    lax.fori_loop(0, model // step, project, 0)
    for copy in pair_copies(sp_count):
        copy.start()
    sum_pairs(sp_count)
    mid_value = (resid_ref[...].astype(f32) + sum_across(sp_count)).astype(bf16).astype(f32)
    middle[...] = mid_value
    x_all[s, t] = (
        mid_value
        * lax.rsqrt(jnp.mean(mid_value * mid_value, axis=1, keepdims=True) + 1e-06)
        * gain_ref[...]
    ).astype(bf16)

    def along_copy(i):
        return remote(
            x_all.at[s, t],
            x_all.at[s, t],
            z_send.at[i],
            z_recv.at[i],
            {"sp": paired(s, i, sp_count)},
        )

    def spread_copies(i):
        block = x_all.at[paired(s, i, sp_count), t]
        return [
            remote(
                block,
                block,
                gx_send.at[i, j - 1],
                gx_recv.at[i, j - 1],
                {"tp": 2 * lax.rem(x + j, width) + c},
            )
            for j in range(1, width)
        ]

    def twin_copy(i, j):
        block = x_all.at[paired(s, i, sp_count), 2 * lax.rem(x - j + width, width) + c]
        return remote(block, block, gs_send.at[i, j], gs_recv.at[i, j], {"tp": sibling})

    def spread(i):
        for copy in spread_copies(i):
            copy.start()
        twin_copy(i, 0).start()

    def return_copy(i):
        return remote(
            z_out.at[i],
            returned.at[i],
            rz_send.at[i],
            rz_recv.at[i],
            {"sp": paired(s, i, sp_count)},
        )

    spread(0)
    for i in range(1, sp_count):
        along_copy(i).start()
    for load in loads[1:]:
        load.wait()

    f_step = 256 if ff % 256 == 0 else ff

    def turn(i, _):
        @pl.when(i + 1 < sp_count)
        def _():
            along_copy(i + 1).wait_recv()
            spread(i + 1)

        @pl.when(i < sp_count)
        def _():
            for j, copy in enumerate(spread_copies(i)):
                copy.wait_recv()
                twin_copy(i, j + 1).start()
            for j in range(width):
                twin_copy(i, j).wait_recv()
            rows_in = x_all[paired(s, i, sp_count)].reshape(tp_count * rows, model)

            def widen(n, _):
                columns = pl.ds(pl.multiple_of(n * f_step, f_step), f_step)
                gate = jnp.dot(rows_in, w_gate[:, columns], preferred_element_type=f32)
                up = jnp.dot(rows_in, w_up[:, columns], preferred_element_type=f32)
                hidden[:, columns] = (gate / (1.0 + jnp.exp(-gate)) * up).astype(bf16)
                return 0

            lax.fori_loop(0, ff // f_step, widen, 0)

            def narrow(n, _):
                columns = pl.ds(pl.multiple_of(n * step, step), step)
                value = jnp.dot(hidden[...], w_down[:, columns], preferred_element_type=f32)
                part[i, :, :, columns] = value.astype(bf16).reshape(tp_count, rows, step)
                return 0

            lax.fori_loop(0, model // step, narrow, 0)
            for copy in pair_copies(i):
                copy.start()

        @pl.when((i >= 1) & (i <= sp_count))
        def _():
            sum_pairs(i - 1)

        @pl.when(i >= 2)
        def _():
            z_out[i - 2] = sum_across(i - 2).astype(bf16)

            @pl.when(i > 2)
            def _():
                return_copy(i - 2).start()

        return 0

    lax.fori_loop(0, sp_count + 2, turn, 0)

    result = middle[...]
    for i in range(sp_count):
        if i > 0:
            return_copy(i).wait_recv()
        chosen = ids_ref[...] == paired(s, i, sp_count)
        gate = jnp.sum(jnp.where(chosen, gates_ref[...], 0.0), axis=1, keepdims=True)
        value = z_out[0] if i == 0 else returned[i]
        result = result + gate * value.astype(f32)
    out_ref[...] = result.astype(bf16)

    for hop in range(sp_count - 1):

        @pl.when(has_right & (s >= hop))
        def _():
            for copy in passed(hop):
                copy.wait_send()

    for i in range(sp_count + 1):
        for copy in pair_copies(i) + across_copies(i):
            copy.wait_send()
    for i in range(sp_count):
        if i > 0:
            along_copy(i).wait_send()
            return_copy(i).wait_send()
        for copy in spread_copies(i):
            copy.wait_send()
        for j in range(width):
            twin_copy(i, j).wait_send()


def fused(
    queries,
    keys,
    values,
    head_bias,
    documents,
    w_out,
    resid,
    norm_gain,
    expert_ids,
    expert_gates,
    w_gate,
    w_up,
    w_down,
):
    sp_count, tp_count = lax.axis_size("sp"), lax.axis_size("tp")
    width = tp_count // 2
    tok = queries.shape[0]
    kv_local = keys.shape[1] // DH
    rep = queries.shape[1] // keys.shape[1]
    rows, model = resid.shape
    ff = w_up.shape[2]
    bf16, f32 = jnp.bfloat16, jnp.float32
    dma = pltpu.SemaphoreType.DMA
    vmem, hbm = pl.BlockSpec(memory_space=pltpu.VMEM), pl.BlockSpec(memory_space=pl.ANY)
    return pl.pallas_call(
        functools.partial(fused_kernel, sp_count, tp_count),
        out_shape=jax.ShapeDtypeStruct((rows, model), bf16),
        in_specs=[vmem] * 3
        + [pl.BlockSpec(memory_space=pltpu.SMEM)]
        + [vmem] * 5
        + [hbm] * 4,
        out_specs=vmem,
        scratch_shapes=[
            pltpu.VMEM(w_out.shape, bf16),
            pltpu.VMEM(w_gate.shape[1:], bf16),
            pltpu.VMEM(w_up.shape[1:], bf16),
            pltpu.VMEM(w_down.shape[1:], bf16),
            pltpu.VMEM((sp_count - 1,) + keys.shape, bf16),
            pltpu.VMEM((sp_count - 1,) + values.shape, bf16),
            pltpu.VMEM((sp_count - 1, 1, tok), jnp.int32),
            pltpu.VMEM((kv_local, rep * tok, DH), f32),
            pltpu.VMEM((kv_local, rep * tok, tok), f32),
            pltpu.VMEM(queries.shape, bf16),
            pltpu.VMEM((rows, model), f32),
            pltpu.VMEM((sp_count, tp_count, rows, model), bf16),
            pltpu.VMEM((tp_count * rows, ff), bf16),
            pltpu.VMEM((sp_count + 1, tp_count, rows, model), bf16),
            pltpu.VMEM((sp_count + 1, width, rows, model), bf16),
            pltpu.VMEM((sp_count + 1, width - 1, rows, model), bf16),
            pltpu.VMEM((sp_count + 1, width - 1, rows, model), bf16),
            pltpu.VMEM((sp_count, rows, model), bf16),
            pltpu.VMEM((sp_count, rows, model), bf16),
            dma((4,)),
            dma((sp_count - 1, 3)),
            dma((sp_count - 1, 3)),
            dma((sp_count,)),
            dma((sp_count,)),
            dma((sp_count, width - 1)),
            dma((sp_count, width - 1)),
            dma((sp_count, width)),
            dma((sp_count, width)),
            dma((sp_count + 1, width)),
            dma((sp_count + 1, width)),
            dma((sp_count + 1, width - 1)),
            dma((sp_count + 1, width - 1)),
            dma((sp_count,)),
            dma((sp_count,)),
        ],
        compiler_params=pltpu.CompilerParams(
            collective_id=0, has_side_effects=True, vmem_limit_bytes=60 * 2**20
        ),
    )(
        queries,
        keys,
        values,
        head_bias,
        documents.reshape(1, tok),
        resid,
        norm_gain.reshape(1, model),
        expert_ids,
        expert_gates,
        w_out,
        w_gate,
        w_up,
        w_down,
    )


def block(*arrays):
    queries, resid, w_gate = arrays[0], arrays[6], arrays[10]
    sp_count, tp_count = lax.axis_size("sp"), lax.axis_size("tp")
    rows = resid.shape[0]
    slots = min(rows, max(2, 2 * TOPK * rows // (w_gate.shape[0] * sp_count)))
    powers = sp_count & (sp_count - 1) == 0 and tp_count % 2 == 0 and min(sp_count, tp_count // 2) > 1
    if slots == rows and w_gate.shape[0] == 1 and powers and queries.shape[0] == DH:
        return fused(*arrays)
    return local(*arrays)


def solution(mesh):
    return jax.shard_map(
        block,
        mesh=mesh,
        in_specs=(
            P(("grp", "sp"), "tp"),
            P(("grp", "sp"), "tp"),
            P(("grp", "sp"), "tp"),
            P("tp"),
            P(("grp", "sp")),
            P("tp", None),
            P(("grp", "sp", "tp"), None),
            P(),
            P(("grp", "sp", "tp"), None),
            P(("grp", "sp", "tp"), None),
            P("sp", None, "tp"),
            P("sp", None, "tp"),
            P("sp", "tp", None),
        ),
        out_specs=P(("grp", "sp", "tp"), None),
        check_vma=False,
    )
```

```python
import functools

import jax
import jax.numpy as jnp
from jax import lax
from jax.experimental import pallas as pl
from jax.experimental.pallas import tpu as pltpu
from jax.sharding import PartitionSpec as P

D = 2048
HEADS = 16
KV_HEADS = 8
DH = 128
TOPK = 2


def passed_along(value, axis, steps):
    count = lax.axis_size(axis)
    initial, last = (max(0, -steps), min(count, count - steps))
    return lax.ppermute(value, axis, [(source, source + steps) for source in range(initial, last)])


def attend_terms(query_grid, bias_grid, key_block, value_block, live, carried):
    kv_local = bias_grid.shape[0]
    key_count = key_block.shape[0]
    logits = (
        jnp.einsum(
            "qgrd,sgd->grqs",
            query_grid,
            key_block.reshape(key_count, kv_local, DH),
            preferred_element_type=jnp.float32,
        )
        * DH ** (-0.5)
        + bias_grid[:, :, None, None]
    )
    keep = jnp.where(live, jax.nn.log_sigmoid(-logits), 0.0)
    after = lax.cumsum(keep, axis=3, reverse=True) - keep + carried[:, :, :, None]
    weight = jnp.where(live, jnp.exp(jax.nn.log_sigmoid(logits) + after), 0.0).astype(jnp.bfloat16)
    partial_mix = jnp.einsum(
        "grqs,sgd->qgrd",
        weight,
        value_block.reshape(key_count, kv_local, DH),
        preferred_element_type=jnp.float32,
    )
    return (partial_mix, jnp.sum(keep, axis=3))


def local(
    queries,
    keys,
    values,
    head_bias,
    documents,
    w_out,
    resid,
    norm_gain,
    expert_ids,
    expert_gates,
    w_gate,
    w_up,
    w_down,
):
    tok_count = queries.shape[0]
    kv_local = keys.shape[1] // DH
    group_size = HEADS // KV_HEADS
    sp_count = lax.axis_size("sp")
    tp_count = lax.axis_size("tp")
    sp_index = lax.axis_index("sp")
    query_grid = queries.reshape(tok_count, kv_local, group_size, DH)
    bias_grid = head_bias.reshape(kv_local, group_size)
    doc_here = documents.astype(jnp.bfloat16)
    doc_column = doc_here.reshape(tok_count, 1)
    local_pos = jnp.arange(tok_count, dtype=jnp.int32)
    live_local = (local_pos[None, :] < local_pos[:, None]) & (
        documents[None, :] == documents[:, None]
    )
    zero_carry = jnp.zeros((kv_local, group_size, tok_count), jnp.float32)
    mix_total, carried = attend_terms(query_grid, bias_grid, keys, values, live_local, zero_carry)

    def visit(turn_index, state):
        mix_sum, carry_sum, key_block, value_block, doc_block = state
        key_block, value_block, doc_block = passed_along(
            (key_block, value_block, doc_block), "sp", 1
        )
        live = (doc_block[:, 0][None, :] == doc_here[:, None]) & (sp_index - turn_index >= 0)
        partial_mix, block_keep = attend_terms(
            query_grid, bias_grid, key_block, value_block, live, carry_sum
        )
        return (mix_sum + partial_mix, carry_sum + block_keep, key_block, value_block, doc_block)

    mix_total, carried, key_last, value_last, doc_last = lax.fori_loop(
        1, sp_count, visit, (mix_total, carried, keys, values, doc_column)
    )
    mixed = mix_total.reshape(tok_count, kv_local * group_size * DH).astype(jnp.bfloat16)
    projected = lax.psum_scatter(
        jnp.dot(mixed, w_out, preferred_element_type=jnp.float32).astype(jnp.bfloat16),
        "tp",
        scatter_dimension=0,
        tiled=True,
    ).astype(jnp.float32)
    middle = (resid.astype(jnp.float32) + projected).astype(jnp.bfloat16)
    middle_value = middle.astype(jnp.float32)
    normed = (
        middle_value
        * lax.rsqrt(jnp.mean(middle_value * middle_value, axis=1, keepdims=True) + 1e-06)
        * norm_gain
    ).astype(jnp.bfloat16)
    row_count = normed.shape[0]
    expert_count = w_gate.shape[0] * sp_count
    slot_limit = min(row_count, max(2, 2 * TOPK * row_count // expert_count))
    flat_ids = expert_ids.reshape(-1)
    onehot_ids = (flat_ids[:, None] == jnp.arange(expert_count, dtype=jnp.int32)[None, :]).astype(
        jnp.int32
    )
    earlier = jnp.cumsum(onehot_ids, axis=0) - onehot_ids
    slot_ids = jnp.sum(earlier * onehot_ids, axis=1)
    target = flat_ids * slot_limit + slot_ids
    placing = (
        jnp.arange(expert_count * slot_limit, dtype=jnp.int32)[:, None] == target[None, :]
    ).astype(jnp.bfloat16)
    by_token = jnp.sum(placing.reshape(expert_count * slot_limit, row_count, TOPK), axis=2)
    outgoing = jnp.dot(by_token, normed, preferred_element_type=jnp.float32).astype(jnp.bfloat16)
    outgoing = outgoing.reshape(expert_count, slot_limit, D)
    arrived = lax.all_to_all(outgoing, "sp", split_axis=0, concat_axis=0, tiled=True)
    gathered = lax.all_gather(arrived, "tp", axis=0, tiled=True)
    expert_rows = gathered.reshape(-1, D)
    gate_value = jnp.dot(expert_rows, w_gate[0], preferred_element_type=jnp.float32)
    up_value = jnp.dot(expert_rows, w_up[0], preferred_element_type=jnp.float32)
    hidden = (jax.nn.silu(gate_value) * up_value).astype(jnp.bfloat16)
    partial_out = jnp.dot(hidden, w_down[0], preferred_element_type=jnp.float32)
    summed = lax.psum_scatter(
        partial_out.reshape(tp_count, sp_count * slot_limit, D).astype(jnp.bfloat16),
        "tp",
        scatter_dimension=0,
        tiled=True,
    ).astype(jnp.float32)
    expert_result = summed.reshape(sp_count, slot_limit, D).astype(jnp.bfloat16)
    returned = lax.all_to_all(expert_result, "sp", split_axis=0, concat_axis=0, tiled=True)
    routed = jnp.dot(placing.T, returned.reshape(-1, D), preferred_element_type=jnp.float32)
    combined = jnp.sum(expert_gates[:, :, None] * routed.reshape(row_count, TOPK, D), axis=1)
    return (middle_value + combined).astype(jnp.bfloat16)


MESH = pl.DeviceIdType.MESH


def paired(index, turn, count):
    result, bit = 0, 1
    while bit < count:
        a, b = lax.rem(index // bit, 2), lax.rem(turn // bit, 2)
        result = result + bit * (a + b - 2 * a * b)
        bit *= 2
    return result


def fused_kernel(
    sp_count,
    tp_count,
    q_ref,
    k_ref,
    v_ref,
    bias_ref,
    doc_ref,
    resid_ref,
    gain_ref,
    ids_ref,
    gates_ref,
    w_out_hbm,
    w_gate_hbm,
    w_up_hbm,
    w_down_hbm,
    out_ref,
    w_out,
    w_gate,
    w_up,
    w_down,
    k_all,
    v_all,
    doc_all,
    mix_acc,
    carry,
    mixed,
    middle,
    x_all,
    hidden,
    part,
    sib_in,
    x_out,
    x_in,
    z_out,
    returned,
    w_sem,
    kv_send,
    kv_recv,
    z_send,
    z_recv,
    gx_send,
    gx_recv,
    gs_send,
    gs_recv,
    ps_send,
    ps_recv,
    px_send,
    px_recv,
    rz_send,
    rz_recv,
):
    s = lax.axis_index("sp")
    t = lax.axis_index("tp")
    width = tp_count // 2
    x, c = t // 2, lax.rem(t, 2)
    sibling = 2 * x + 1 - c
    tok = q_ref.shape[0]
    kv_local = k_ref.shape[1] // DH
    rep = q_ref.shape[1] // k_ref.shape[1]
    rows, model = resid_ref.shape
    ff = w_up.shape[1]
    f32, bf16 = jnp.float32, jnp.bfloat16

    loads = [
        pltpu.make_async_copy(src, dst, w_sem.at[j])
        for j, (src, dst) in enumerate(
            (
                (w_out_hbm, w_out),
                (w_gate_hbm.at[0], w_gate),
                (w_up_hbm.at[0], w_up),
                (w_down_hbm.at[0], w_down),
            )
        )
    ]
    for load in loads:
        load.start()

    barrier = pltpu.get_barrier_semaphore()
    for j in range(1, sp_count):
        pl.semaphore_signal(
            barrier, inc=1, device_id={"sp": lax.rem(s + j, sp_count)}, device_id_type=MESH
        )
    for j in range(1, tp_count):
        pl.semaphore_signal(
            barrier, inc=1, device_id={"tp": lax.rem(t + j, tp_count)}, device_id_type=MESH
        )
    pl.semaphore_wait(barrier, sp_count + tp_count - 2)

    def remote(src, dst, send, recv, device):
        return pltpu.make_async_remote_copy(
            src_ref=src,
            dst_ref=dst,
            send_sem=send,
            recv_sem=recv,
            device_id=device,
            device_id_type=MESH,
        )

    lane_pieces = [slice(g * DH, (g + 1) * DH) for g in range(kv_local)]

    def passed(hop):
        right = {"sp": lax.rem(s + 1, sp_count)}
        pairs = [(doc_ref if hop == 0 else doc_all.at[hop - 1], doc_all.at[hop])]
        for own, slots in ((k_ref, k_all), (v_ref, v_all)):
            for lanes in lane_pieces:
                source = own.at[:, lanes] if hop == 0 else slots.at[hop - 1, :, lanes]
                pairs.append((source, slots.at[hop, :, lanes]))
        return [
            remote(src, dst, kv_send.at[hop, j], kv_recv.at[hop, j], right)
            for j, (src, dst) in enumerate(pairs)
        ]

    has_right = s < sp_count - 1

    @pl.when(has_right)
    def _():
        for copy in passed(0):
            copy.start()

    at_row = lax.broadcasted_iota(jnp.int32, (tok, tok), 0)
    at_col = lax.broadcasted_iota(jnp.int32, (tok, tok), 1)
    summing = jnp.concatenate(
        [(at_row > at_col).astype(f32), jnp.ones((tok, tok), f32)], axis=1
    ).astype(bf16)
    doc_query = jnp.broadcast_to(doc_ref[...].astype(f32), (tok, tok)).T

    def attend(hop):
        docs = doc_ref[...] if hop == 0 else doc_all[hop - 1]
        live = doc_query == jnp.broadcast_to(docs.astype(f32), (tok, tok))
        if hop == 0:
            live = live & (at_col < at_row)
        live_f = jnp.concatenate([live.astype(f32)] * rep, axis=0)
        live_all = live_f > 0.5
        for g in range(kv_local):
            heads = [g * rep + r for r in range(rep)]
            query = jnp.concatenate([q_ref[:, h * DH : (h + 1) * DH] for h in heads], axis=0)
            bias = jnp.concatenate([jnp.full((tok, tok), bias_ref[h], f32) for h in heads], axis=0)
            lanes = slice(g * DH, (g + 1) * DH)
            key = k_ref[:, lanes] if hop == 0 else k_all[hop - 1, :, lanes]
            value = v_ref[:, lanes] if hop == 0 else v_all[hop - 1, :, lanes]
            logits = (
                lax.dot_general(
                    query, key, (((1,), (1,)), ((), ())), preferred_element_type=f32
                )
                * DH ** (-0.5)
                + bias
            )
            keep_any = -(jnp.maximum(logits, 0.0) + jnp.log1p(jnp.exp(-jnp.abs(logits))))
            keep = jnp.where(live_all, keep_any, 0.0)
            high = keep.astype(bf16)
            rest = keep - high.astype(f32)
            mid = rest.astype(bf16)
            low = (rest - mid.astype(f32)).astype(bf16)
            sums = (
                jnp.dot(high, summing, preferred_element_type=f32)
                + jnp.dot(mid, summing, preferred_element_type=f32)
                + jnp.dot(low, summing, preferred_element_type=f32)
            )
            after, total = sums[:, :tok], sums[:, tok:]
            if hop > 0:
                after = after + carry[g]
                total = total + carry[g]
            carry[g] = total
            weight = jnp.where(live_all, jnp.exp(logits + keep_any + after), 0.0).astype(bf16)
            mix = jnp.dot(weight, value, preferred_element_type=f32)
            mix_acc[g] = mix if hop == 0 else mix_acc[g] + mix

    attend(0)
    for hop in range(1, sp_count):

        @pl.when(s >= hop)
        def _():
            onward = passed(hop) if hop < sp_count - 1 else None
            for j, copy in enumerate(passed(hop - 1)):
                copy.wait_recv()
                if onward is not None:
                    pl.when(has_right)(onward[j].start)

            attend(hop)

    for g in range(kv_local):
        for r in range(rep):
            h = g * rep + r
            mixed[:, h * DH : (h + 1) * DH] = mix_acc[g, r * tok : (r + 1) * tok, :].astype(bf16)

    cuts = 2
    span = model // cuts
    cols = [slice(h * span, (h + 1) * span) for h in range(cuts)]

    def pair_copies(i, h):
        return [
            remote(
                part.at[i, 2 * j + 1 - c, :, cols[h]],
                sib_in.at[i, j, :, cols[h]],
                ps_send.at[i, j, h],
                ps_recv.at[i, j, h],
                {"tp": sibling},
            )
            for j in range(width)
        ]

    def across_copies(i, h):
        return [
            remote(
                x_out.at[i, j - 1, :, cols[h]],
                x_in.at[i, j - 1, :, cols[h]],
                px_send.at[i, j - 1, h],
                px_recv.at[i, j - 1, h],
                {"tp": 2 * lax.rem(x + j, width) + c},
            )
            for j in range(1, width)
        ]

    def pair_sum(i, at, h):
        return part[i, 2 * at + c, :, cols[h]].astype(f32) + sib_in[i, at, :, cols[h]].astype(f32)

    def sum_pairs(i):
        for h in range(cuts):
            for copy in pair_copies(i, h):
                copy.wait_recv()
            for j, copy in enumerate(across_copies(i, h)):
                x_out[i, j, :, cols[h]] = pair_sum(i, lax.rem(x + j + 1, width), h).astype(bf16)
                copy.start()

    def sum_across(i, h):
        result = pair_sum(i, x, h)
        for j, copy in enumerate(across_copies(i, h)):
            copy.wait_recv()
            result = result + x_in[i, j, :, cols[h]].astype(f32)
        return result

    loads[0].wait()
    step = 512 if span % 512 == 0 else span
    steps = span // step

    def into_part(i, left, right):
        for h in range(cuts):

            def piece(n, _):
                columns = pl.ds(pl.multiple_of(n * step, step), step)
                value = jnp.dot(left[...], right[:, columns], preferred_element_type=f32)
                part[i, :, :, columns] = value.astype(bf16).reshape(tp_count, rows, step)
                return 0

            lax.fori_loop(h * steps, (h + 1) * steps, piece, 0)
            for copy in pair_copies(i, h):
                copy.start()

    into_part(sp_count, mixed, w_out)
    sum_pairs(sp_count)
    for h in range(cuts):
        middle[:, cols[h]] = (
            (resid_ref[:, cols[h]].astype(f32) + sum_across(sp_count, h)).astype(bf16).astype(f32)
        )
    mid_value = middle[...]
    x_all[s, t] = (
        mid_value
        * lax.rsqrt(jnp.mean(mid_value * mid_value, axis=1, keepdims=True) + 1e-06)
        * gain_ref[...]
    ).astype(bf16)

    def group(i):
        return paired(s, lax.rem(sp_count - i, sp_count), sp_count)

    def along_copy(i, h):
        block = x_all.at[s, t, :, cols[h]]
        return remote(block, block, z_send.at[i, h], z_recv.at[i, h], {"sp": group(i)})

    def spread_copies(i, h):
        block = x_all.at[group(i), t, :, cols[h]]
        return [
            remote(
                block,
                block,
                gx_send.at[i, j - 1, h],
                gx_recv.at[i, j - 1, h],
                {"tp": 2 * lax.rem(x + j, width) + c},
            )
            for j in range(1, width)
        ]

    def twin_copy(i, j, h):
        block = x_all.at[group(i), 2 * lax.rem(x - j + width, width) + c, :, cols[h]]
        return remote(block, block, gs_send.at[i, j, h], gs_recv.at[i, j, h], {"tp": sibling})

    def spread(i, h):
        for copy in spread_copies(i, h):
            copy.start()
        twin_copy(i, 0, h).start()

    def return_copy(i, h):
        return remote(
            z_out.at[i, :, cols[h]],
            returned.at[i, :, cols[h]],
            rz_send.at[i, h],
            rz_recv.at[i, h],
            {"sp": group(i)},
        )

    for h in range(cuts):
        for i in range(1, sp_count):
            along_copy(i, h).start()
        spread(0, h)
    for load in loads[1:]:
        load.wait()

    f_step = 256 if ff % 256 == 0 else ff

    def turn(i, _):
        @pl.when(i + 1 < sp_count)
        def _():
            for h in range(cuts):
                along_copy(i + 1, h).wait_recv()
                spread(i + 1, h)

        @pl.when(i < sp_count)
        def _():
            for h in range(cuts):
                for j, copy in enumerate(spread_copies(i, h)):
                    copy.wait_recv()
                    twin_copy(i, j + 1, h).start()
            for h in range(cuts):
                for j in range(width):
                    twin_copy(i, j, h).wait_recv()

        @pl.when(i < sp_count)
        def _():
            rows_in = x_all[group(i)].reshape(tp_count * rows, model)

            def widen(n, _):
                columns = pl.ds(pl.multiple_of(n * f_step, f_step), f_step)
                gate = jnp.dot(rows_in, w_gate[:, columns], preferred_element_type=f32)
                up = jnp.dot(rows_in, w_up[:, columns], preferred_element_type=f32)
                hidden[:, columns] = (gate / (1.0 + jnp.exp(-gate)) * up).astype(bf16)
                return 0

            lax.fori_loop(0, ff // f_step, widen, 0)
            into_part(i, hidden, w_down)

        @pl.when((i >= 1) & (i <= sp_count))
        def _():
            sum_pairs(i - 1)

        @pl.when(i >= 2)
        def _():
            for h in range(cuts):
                z_out[i - 2, :, cols[h]] = sum_across(i - 2, h).astype(bf16)
                pl.when(i > 2)(return_copy(i - 2, h).start)

        return 0

    lax.fori_loop(0, sp_count + 2, turn, 0)

    diagonal = lax.broadcasted_iota(jnp.int32, (rows, rows), 0) == lax.broadcasted_iota(
        jnp.int32, (rows, rows), 1
    )
    for i in range(sp_count):
        chosen = ids_ref[...] == group(i)
        gate_row = jnp.sum(jnp.where(chosen, gates_ref[...], 0.0), axis=0, keepdims=True)
        gate = jnp.sum(
            jnp.where(diagonal, jnp.broadcast_to(gate_row, (rows, rows)), 0.0), axis=1, keepdims=True
        )
        for h in range(cuts):
            if i > 0:
                return_copy(i, h).wait_recv()
            value = z_out[0, :, cols[h]] if i == 0 else returned[i, :, cols[h]]
            middle[:, cols[h]] = middle[:, cols[h]] + gate * value.astype(f32)
    out_ref[...] = middle[...].astype(bf16)

    for hop in range(sp_count - 1):

        @pl.when(has_right & (s >= hop))
        def _():
            for copy in passed(hop):
                copy.wait_send()

    def drain(i, _):
        for h in range(cuts):
            for copy in pair_copies(i, h) + across_copies(i, h):
                copy.wait_send()

            @pl.when(i < sp_count)
            def _():
                for copy in spread_copies(i, h):
                    copy.wait_send()
                for j in range(width):
                    twin_copy(i, j, h).wait_send()

            @pl.when((i >= 1) & (i < sp_count))
            def _():
                along_copy(i, h).wait_send()
                return_copy(i, h).wait_send()

        return 0

    lax.fori_loop(0, sp_count + 1, drain, 0)


def fused(
    queries,
    keys,
    values,
    head_bias,
    documents,
    w_out,
    resid,
    norm_gain,
    expert_ids,
    expert_gates,
    w_gate,
    w_up,
    w_down,
):
    sp_count, tp_count = lax.axis_size("sp"), lax.axis_size("tp")
    width = tp_count // 2
    tok = queries.shape[0]
    kv_local = keys.shape[1] // DH
    rep = queries.shape[1] // keys.shape[1]
    rows, model = resid.shape
    ff = w_up.shape[2]
    bf16, f32 = jnp.bfloat16, jnp.float32
    dma = pltpu.SemaphoreType.DMA
    vmem, hbm = pl.BlockSpec(memory_space=pltpu.VMEM), pl.BlockSpec(memory_space=pl.ANY)
    return pl.pallas_call(
        functools.partial(fused_kernel, sp_count, tp_count),
        out_shape=jax.ShapeDtypeStruct((rows, model), bf16),
        in_specs=[vmem] * 3
        + [pl.BlockSpec(memory_space=pltpu.SMEM)]
        + [vmem] * 5
        + [hbm] * 4,
        out_specs=vmem,
        scratch_shapes=[
            pltpu.VMEM(w_out.shape, bf16),
            pltpu.VMEM(w_gate.shape[1:], bf16),
            pltpu.VMEM(w_up.shape[1:], bf16),
            pltpu.VMEM(w_down.shape[1:], bf16),
            pltpu.VMEM((sp_count - 1,) + keys.shape, bf16),
            pltpu.VMEM((sp_count - 1,) + values.shape, bf16),
            pltpu.VMEM((sp_count - 1, 1, tok), jnp.int32),
            pltpu.VMEM((kv_local, rep * tok, DH), f32),
            pltpu.VMEM((kv_local, rep * tok, tok), f32),
            pltpu.VMEM(queries.shape, bf16),
            pltpu.VMEM((rows, model), f32),
            pltpu.VMEM((sp_count, tp_count, rows, model), bf16),
            pltpu.VMEM((tp_count * rows, ff), bf16),
            pltpu.VMEM((sp_count + 1, tp_count, rows, model), bf16),
            pltpu.VMEM((sp_count + 1, width, rows, model), bf16),
            pltpu.VMEM((sp_count + 1, width - 1, rows, model), bf16),
            pltpu.VMEM((sp_count + 1, width - 1, rows, model), bf16),
            pltpu.VMEM((sp_count, rows, model), bf16),
            pltpu.VMEM((sp_count, rows, model), bf16),
            dma((4,)),
            dma((sp_count - 1, 2 * kv_local + 1)),
            dma((sp_count - 1, 2 * kv_local + 1)),
            dma((sp_count, 2)),
            dma((sp_count, 2)),
            dma((sp_count, width - 1, 2)),
            dma((sp_count, width - 1, 2)),
            dma((sp_count, width, 2)),
            dma((sp_count, width, 2)),
            dma((sp_count + 1, width, 2)),
            dma((sp_count + 1, width, 2)),
            dma((sp_count + 1, width - 1, 2)),
            dma((sp_count + 1, width - 1, 2)),
            dma((sp_count, 2)),
            dma((sp_count, 2)),
        ],
        compiler_params=pltpu.CompilerParams(
            collective_id=0, has_side_effects=True, vmem_limit_bytes=60 * 2**20
        ),
    )(
        queries,
        keys,
        values,
        head_bias,
        documents.reshape(1, tok),
        resid,
        norm_gain.reshape(1, model),
        expert_ids.T,
        expert_gates.T,
        w_out,
        w_gate,
        w_up,
        w_down,
    )


def block(*arrays):
    queries, resid, w_gate = arrays[0], arrays[6], arrays[10]
    sp_count, tp_count = lax.axis_size("sp"), lax.axis_size("tp")
    rows = resid.shape[0]
    slots = min(rows, max(2, 2 * TOPK * rows // (w_gate.shape[0] * sp_count)))
    powers = sp_count & (sp_count - 1) == 0 and tp_count % 2 == 0 and min(sp_count, tp_count // 2) > 1
    if slots == rows and w_gate.shape[0] == 1 and powers and queries.shape[0] == DH:
        return fused(*arrays)
    return local(*arrays)


def solution(mesh):
    return jax.shard_map(
        block,
        mesh=mesh,
        in_specs=(
            P(("grp", "sp"), "tp"),
            P(("grp", "sp"), "tp"),
            P(("grp", "sp"), "tp"),
            P("tp"),
            P(("grp", "sp")),
            P("tp", None),
            P(("grp", "sp", "tp"), None),
            P(),
            P(("grp", "sp", "tp"), None),
            P(("grp", "sp", "tp"), None),
            P("sp", None, "tp"),
            P("sp", None, "tp"),
            P("sp", "tp", None),
        ),
        out_specs=P(("grp", "sp", "tp"), None),
        check_vma=False,
    )
```
